32 devices in a mesh: tp: 16 (over z, y, x), dp: 2 (over core).
Axes of the slice: x: 2, y: 2, z: 4, core: 2. Of those that a mesh axis runs over, the one named last changes fastest.
Arguments:
- tokens: bfloat16 [256, 4096], P(None, 'dp'), may hold values from -20 to 20
- norm_gain: float32 [2, 4096], P(None, 'dp'), may hold values from 0.1 to 1.9
- receptance: bfloat16 [2, 4096, 1024], P(None, 'dp', 'tp'), may hold values from -0.09375 to 0.09375
- key_proj: bfloat16 [2, 4096, 1024], P(None, 'dp', 'tp'), may hold values from -0.09375 to 0.09375
- value_proj: bfloat16 [2, 4096, 1024], P(None, 'dp', 'tp'), may hold values from -0.09375 to 0.09375
- decay_proj: bfloat16 [2, 4096, 1024], P(None, 'dp', 'tp'), may hold values from -0.09375 to 0.09375
- rate_proj: bfloat16 [2, 4096, 1024], P(None, 'dp', 'tp'), may hold values from -0.09375 to 0.09375
- gate_proj: bfloat16 [2, 4096, 1024], P(None, 'dp', 'tp'), may hold values from -0.09375 to 0.09375
- decay_base: float32 [2, 1024], P(None, 'tp'), may hold values from -6 to 1
- group_gain: float32 [2, 1024], P(None, 'tp'), may hold values from 0.1 to 1.9
- output_proj: bfloat16 [2, 1024, 4096], P(None, 'tp', 'dp'), may hold values from -0.1875 to 0.1875
- state: float32 [2, 256, 16, 4096], P(None, 'dp', 'tp'), may hold values from -3 to 3
Outputs:
- next_tokens: bfloat16 [256, 4096], P(None, 'dp')
- new_state: float32 [2, 256, 16, 4096], P(None, 'dp', 'tp')
The draws below stay inside these ranges and needn't reach their ends.
All inputs are finite; a program needn't handle non-finite values.
Results may differ from the reference program's by a relative error of at most 0.0066.
Values may be sent and summed in bfloat16 or wider, within the bound.
A program may use at most 64 MiB of HBM per device.

```python
import jax
import jax.numpy as jnp
from jax import lax

D = 4096
HEAD = 64
HEADS = 16
D_ATT = 1024
LAYERS = 2
BATCH = 256


def draw_tokens(key, part):
    base_key, row_key = jax.random.split(key)
    position = jnp.arange(D, dtype=jnp.float32) / D
    feature_scale = 0.4 + 1.6 * position
    row_scale = jnp.exp(jax.random.uniform(row_key, (BATCH, 1), jnp.float32, -0.6, 0.6))
    values = jnp.clip(jax.random.normal(base_key, (BATCH, D), jnp.float32), -5.0, 5.0)
    return (values * feature_scale[None, :] * row_scale).astype(jnp.bfloat16)


def block_levels(stream_key, shape, pieces, low, high):
    def one(axis_at, blocks):
        draws = jax.random.uniform(jax.random.fold_in(jax.random.fold_in(stream_key, 6), axis_at), (blocks,), jnp.float32, low / len(pieces), high / len(pieces))
        return jnp.repeat(jnp.exp(draws), shape[axis_at] // blocks).reshape((-1,) + (1,) * (len(shape) - axis_at - 1))

    level = one(*pieces[0])
    for cut in pieces[1:]:
        level = level * one(*cut)
    return level


def gaussian(stream_key, shape, deviation, limit, cuts=(), held_as=jnp.bfloat16):
    loudness = block_levels(stream_key, shape, cuts, -0.22, 0.18) if cuts else 1.0
    drawn = jax.random.normal(stream_key, shape, jnp.float32) * deviation * loudness
    return jnp.minimum(jnp.maximum(drawn, -limit), limit).astype(held_as)


def setup_inputs(seed: int = 0) -> dict:
    arg_keys = jax.random.split(jax.random.key(seed), 13)
    return {
        "tokens": draw_tokens(jax.random.fold_in(arg_keys[12], 71), 0),
        "norm_gain": jnp.clip(1.0 + 0.18 * jax.random.normal(arg_keys[1], (LAYERS, D), jnp.float32), 0.1, 1.9),
        "receptance": gaussian(arg_keys[2], (LAYERS, D, D_ATT), D ** -0.5, 0.09375, ((1, 2), (2, 16))),
        "key_proj": gaussian(arg_keys[3], (LAYERS, D, D_ATT), D ** -0.5, 0.09375, ((1, 2), (2, 16))),
        "value_proj": gaussian(arg_keys[4], (LAYERS, D, D_ATT), D ** -0.5, 0.09375, ((1, 2), (2, 16))),
        "decay_proj": gaussian(arg_keys[5], (LAYERS, D, D_ATT), D ** -0.5, 0.09375, ((1, 2), (2, 16))),
        "rate_proj": gaussian(arg_keys[6], (LAYERS, D, D_ATT), D ** -0.5, 0.09375, ((1, 2), (2, 16))),
        "gate_proj": gaussian(arg_keys[7], (LAYERS, D, D_ATT), D ** -0.5, 0.09375, ((1, 2), (2, 16))),
        "decay_base": jnp.clip(-6.0 + 7.0 * jax.random.uniform(arg_keys[8], (LAYERS, D_ATT), jnp.float32) ** block_levels(arg_keys[8], (LAYERS, D_ATT), ((1, 16),), -0.2, 0.2), -6.0, 1.0),
        "group_gain": jnp.clip(1.0 + 0.18 * jax.random.normal(arg_keys[9], (LAYERS, D_ATT), jnp.float32), 0.1, 1.9),
        "output_proj": gaussian(arg_keys[10], (LAYERS, D_ATT, D), D_ATT ** -0.5, 0.1875, ((1, 16), (2, 2))),
        "state": gaussian(arg_keys[11], (LAYERS, BATCH, HEADS, HEAD * HEAD), 0.5, 3.0, ((1, 2), (2, 16)), jnp.float32),
    }


norm_floor = 0.1
group_floor = 0.5

def recurrence(state_block, recept_heads, key_heads, value_heads, decay_heads, rate_heads):
    log_rate = -jax.nn.softplus(-decay_heads) - 0.5
    forget = jnp.exp(-jnp.exp(log_rate))
    learn_rate = jax.nn.sigmoid(rate_heads)
    unit_key = key_heads * lax.rsqrt(lax.optimization_barrier(jnp.sum(key_heads * key_heads, axis=-1, keepdims=True)) + 1.0)
    scaled = key_heads * learn_rate
    removed = jnp.einsum('bhvk,bhk->bhv', state_block, -unit_key, precision=lax.Precision.HIGHEST)
    updated = state_block * forget[:, :, None, :] + removed[..., None] * (unit_key * learn_rate)[:, :, None, :] + value_heads[..., None] * scaled[:, :, None, :]
    read_out = jnp.einsum('bhvk,bhk->bhv', updated, recept_heads, precision=lax.Precision.HIGHEST)
    centre = read_out - lax.optimization_barrier(jnp.mean(read_out, axis=-1, keepdims=True))
    normal = centre * lax.rsqrt(lax.optimization_barrier(jnp.mean(centre * centre, axis=-1, keepdims=True)) + group_floor)
    return (updated, normal)

def reference(tokens, norm_gain, receptance, key_proj, value_proj, decay_proj, rate_proj, gate_proj, decay_base, group_gain, output_proj, state):
    current = tokens
    finals = []
    for section_index in range(LAYERS):
        floats = current.astype(jnp.float32)
        squares = lax.optimization_barrier(jnp.sum(floats * floats, axis=1))
        inv_rms = lax.rsqrt(squares / D + norm_floor)
        normed = (floats * norm_gain[section_index]).astype(jnp.bfloat16)

        def by_head(weights):
            term = jnp.dot(normed, weights[section_index], preferred_element_type=jnp.float32)
            rounded = lax.optimization_barrier((inv_rms[:, None] * term).astype(jnp.bfloat16))
            return rounded.astype(jnp.float32).reshape(BATCH, HEADS, HEAD)
        decay_heads = by_head(decay_proj) + decay_base[section_index].reshape(1, HEADS, HEAD)
        updated, normal = recurrence(state[section_index].reshape(BATCH, HEADS, HEAD, HEAD), by_head(receptance), by_head(key_proj), by_head(value_proj), decay_heads, by_head(rate_proj))
        finals.append(updated.reshape(BATCH, HEADS, HEAD * HEAD))
        gate_value = jax.nn.sigmoid(by_head(gate_proj).reshape(BATCH, D_ATT))
        mixed_heads = (normal.reshape(BATCH, D_ATT) * group_gain[section_index] * gate_value).astype(jnp.bfloat16)
        branch = jnp.dot(mixed_heads, output_proj[section_index], preferred_element_type=jnp.float32)
        current = (floats + branch).astype(jnp.bfloat16)
    return (current, jnp.stack(finals))
```

```python
import functools

import jax
import jax.numpy as jnp
from jax import lax
from jax.experimental import pallas as pl
from jax.experimental.pallas import tpu as pltpu
from jax.sharding import PartitionSpec as P

D = 4096
HEAD = 64
LAYERS = 2


norm_floor = 0.1
group_floor = 0.5


def recurrence(state_block, recept_heads, key_heads, value_heads, decay_heads, rate_heads):
    log_rate = -jax.nn.softplus(-decay_heads) - 0.5
    forget = jnp.exp(-jnp.exp(log_rate))
    learn_rate = jax.nn.sigmoid(rate_heads)
    unit_key = key_heads * lax.rsqrt(jnp.sum(key_heads * key_heads, axis=-1, keepdims=True) + 1.0)
    scaled = key_heads * learn_rate
    removed = jnp.einsum("bhvk,bhk->bhv", state_block, -unit_key, precision=lax.Precision.HIGHEST)
    updated = (
        state_block * forget[:, :, None, :]
        + removed[..., None] * (unit_key * learn_rate)[:, :, None, :]
        + value_heads[..., None] * scaled[:, :, None, :]
    )
    read_out = jnp.einsum("bhvk,bhk->bhv", updated, recept_heads, precision=lax.Precision.HIGHEST)
    centre = read_out - jnp.mean(read_out, axis=-1, keepdims=True)
    normal = centre * lax.rsqrt(jnp.mean(centre * centre, axis=-1, keepdims=True) + group_floor)
    return (updated, normal)


def shards(
    tokens,
    norm_gain,
    receptance,
    key_proj,
    value_proj,
    decay_proj,
    rate_proj,
    gate_proj,
    decay_base,
    group_gain,
    output_proj,
    state,
):
    local_rows = state.shape[1]
    first_row = lax.axis_index("dp") * local_rows
    local_heads = state.shape[2]
    current = tokens
    finals = []
    for section_index in range(LAYERS):
        floats = current.astype(jnp.float32)
        squares = jnp.sum(floats * floats, axis=1)
        normed = (floats * norm_gain[section_index]).astype(jnp.bfloat16)
        part_recept = jnp.dot(normed, receptance[section_index], preferred_element_type=jnp.float32)
        part_key = jnp.dot(normed, key_proj[section_index], preferred_element_type=jnp.float32)
        part_value = jnp.dot(normed, value_proj[section_index], preferred_element_type=jnp.float32)
        part_decay = jnp.dot(normed, decay_proj[section_index], preferred_element_type=jnp.float32)
        part_rate = jnp.dot(normed, rate_proj[section_index], preferred_element_type=jnp.float32)
        part_gate = jnp.dot(normed, gate_proj[section_index], preferred_element_type=jnp.float32)
        totals = lax.psum(squares, "dp")
        own_squares = lax.dynamic_slice_in_dim(totals, first_row, local_rows, 0)
        summed = (
            lax.psum_scatter(part_recept, "dp", scatter_dimension=0, tiled=True),
            lax.psum_scatter(part_key, "dp", scatter_dimension=0, tiled=True),
            lax.psum_scatter(part_value, "dp", scatter_dimension=0, tiled=True),
            lax.psum_scatter(part_decay, "dp", scatter_dimension=0, tiled=True),
            lax.psum_scatter(part_rate, "dp", scatter_dimension=0, tiled=True),
            lax.psum_scatter(part_gate, "dp", scatter_dimension=0, tiled=True),
        )
        inv_rms = lax.rsqrt(own_squares / D + norm_floor)

        def by_head(term):
            rounded = lax.optimization_barrier((inv_rms[:, None] * term).astype(jnp.bfloat16))
            return rounded.astype(jnp.float32).reshape(local_rows, local_heads, HEAD)

        decay_heads = by_head(summed[3]) + decay_base[section_index].reshape(1, local_heads, HEAD)
        updated, normal = recurrence(
            state[section_index].reshape(local_rows, local_heads, HEAD, HEAD),
            by_head(summed[0]),
            by_head(summed[1]),
            by_head(summed[2]),
            decay_heads,
            by_head(summed[4]),
        )
        finals.append(updated.reshape(local_rows, local_heads, HEAD * HEAD))
        gate_value = jax.nn.sigmoid(by_head(summed[5]).reshape(local_rows, local_heads * HEAD))
        mixed_heads = (
            normal.reshape(local_rows, local_heads * HEAD) * group_gain[section_index] * gate_value
        ).astype(jnp.bfloat16)
        weights_out = output_proj[section_index]

        def apply_out(piece, begin, weights_out=weights_out):
            return jnp.dot(piece, weights_out, preferred_element_type=jnp.float32)

        partial_out = apply_out(lax.all_gather(mixed_heads, "dp", axis=0, tiled=True), jnp.int32(0))
        total = lax.psum(partial_out, "tp")
        current = (floats + total).astype(jnp.bfloat16)
    return (current, jnp.stack(finals))


MESH = pl.DeviceIdType.MESH
NT = (((1,), (1,)), ((), ()))
VMEM_LIMIT = 60 * 1024 * 1024


def remote(src, dst, send, recv, t, d):
    return pltpu.make_async_remote_copy(
        src_ref=src, dst_ref=dst, send_sem=send, recv_sem=recv, device_id={"tp": t, "dp": d}, device_id_type=MESH
    )


def greet(peers):
    barrier = pltpu.get_barrier_semaphore()
    for t, d in peers:
        pl.semaphore_signal(barrier, inc=1, device_id={"tp": t, "dp": d}, device_id_type=MESH)
    pl.semaphore_wait(barrier, len(peers))


class Lanes:
    def __init__(self, tp):
        self.t, self.d = lax.axis_index("tp"), lax.axis_index("dp")
        self.nz = tp // 4
        self.x, self.y, self.z = lax.rem(self.t, 2), lax.rem(self.t // 2, 2), self.t // 4

    def at(self, x, y, dz):
        return lax.rem(self.z + dz, self.nz) * 4 + y * 2 + x

    def peers(self):
        near = [self.at(1 - self.x, self.y, 0), self.at(self.x, 1 - self.y, 0)]
        return [(p, self.d) for p in near + [self.at(self.x, self.y, dz) for dz in range(1, self.nz)]]


def gather(lanes, buf, send, recv):
    x, y, nz, d = lanes.x, lanes.y, lanes.nz, lanes.d
    xp, yp = lanes.at(1 - x, y, 0), lanes.at(x, 1 - y, 0)
    started = []
    count = [0, 0]

    def put(half, block, target):
        op = remote(buf.at[half, block], buf.at[half, block], send.at[half, count[half]], recv.at[half, block], target, d)
        count[half] += 1
        op.start()
        started.append(op)

    def got(half, block):
        remote(buf.at[half, block], buf.at[half, block], send.at[half, 0], recv.at[half, block], xp, d).wait_recv()

    zs = list(range(1, nz))
    own = lanes.t
    put(0, own, yp)
    for dz in zs:
        put(1, own, lanes.at(x, y, dz))
        put(0, own, lanes.at(x, y, dz))
    put(1, own, xp)
    put(1, own, yp)
    put(0, own, xp)
    got(0, yp)
    for dz in zs:
        put(0, yp, lanes.at(x, y, dz))
    put(0, yp, xp)
    got(1, xp)
    put(1, xp, yp)
    for dz in zs:
        block = lanes.at(x, y, dz)
        got(1, block)
        put(1, block, xp)
        put(1, block, yp)
        got(0, block)
        put(0, block, xp)
    for dz in zs:
        block = lanes.at(x, 1 - y, dz)
        got(0, block)
        put(0, block, xp)
        block = lanes.at(1 - x, y, dz)
        got(1, block)
        put(1, block, yp)
    for dz in range(nz):
        for k in range(2):
            got(0, lanes.at(1 - x, k, dz))
            got(1, lanes.at(k, 1 - y, dz))
    for op in started:
        op.wait_send()


def first_kernel(
    tp, tok, gain, wr, wk, wv, wd, wa, wg, wo, proj, near, w1, gain1, outw,
    tokv, w0, part, inbox, load, send, recv, a2a_send, a2a_recv,
):
    lanes = Lanes(tp)
    t, d = lanes.t, lanes.d
    per = tp // 2
    rows, feats = tok.shape
    mine = rows // 2
    cols = feats // per
    weights = (wr, wk, wv, wd, wa, wg)
    loads = [pltpu.make_async_copy(tok, tokv, load.at[0])]
    for i, w in enumerate(weights):
        loads.append(pltpu.make_async_copy(w.at[0], w0.at[pl.ds(i * HEAD, HEAD)], load.at[1 + i]))
        loads.append(pltpu.make_async_copy(w.at[1], w1.at[d, pl.ds(i * HEAD, HEAD)], load.at[7 + i]))
    for op in loads:
        op.start()
    greet([(lax.rem(t + k, tp), d) for k in range(1, tp)] + [(t, 1 - d)])

    def spread(c):
        target = d * per + c
        return remote(wo.at[:, :, pl.ds(c * cols, cols)], outw.at[t], a2a_send.at[c], a2a_recv.at[t], target, d)

    for c in range(per):
        @pl.when(d * per + c != t)
        def _(c=c):
            spread(c).start()

        @pl.when(d * per + c == t)
        def _(c=c):
            pltpu.make_async_copy(wo.at[:, :, pl.ds(c * cols, cols)], outw.at[t], a2a_send.at[c]).start()

    loads[0].wait()
    slot = lax.rem(t, per)
    there = (1 - d) * mine
    pair = [
        remote(
            tokv.at[pl.ds(pl.multiple_of(there, mine), mine), pl.ds(pl.multiple_of(slot * cols, cols), cols)],
            near, send.at[0], recv.at[0], t, 1 - d,
        ),
        remote(gain, gain1.at[d], send.at[1], recv.at[1], t, 1 - d),
    ]
    for i, w in enumerate(weights):
        pair.append(remote(w.at[1], w1.at[d, pl.ds(i * HEAD, HEAD)], send.at[2 + i], recv.at[2 + i], t, 1 - d))
    pair[0].start()
    pair[1].start()
    gain1[pl.ds(d, 1)] = gain[...][None]

    floats = tokv[...].astype(jnp.float32)
    squares = jnp.sum(floats * floats, axis=1, keepdims=True)
    normed = (floats * gain[0:1, :]).astype(jnp.bfloat16)
    for i in range(6):
        loads[1 + 2 * i].wait()
    width = 6 * HEAD
    part[:, 0:width] = lax.dot_general(normed, w0[...], NT, preferred_element_type=jnp.float32)
    part[:, width:] = jnp.broadcast_to(squares, (rows, part.shape[1] - width))
    swap = remote(part.at[pl.ds(pl.multiple_of(there, mine), mine)], inbox, send.at[8], recv.at[8], t, 1 - d)
    swap.start()
    for op in pair[2:]:
        op.start()
    swap.wait_recv()
    total = part[pl.ds(pl.multiple_of(d * mine, mine), mine), :] + inbox[...]
    inv = lax.rsqrt(total[:, width : width + 1] / (feats * 2) + norm_floor)
    proj[...] = (inv * total[:, :width]).astype(jnp.bfloat16)

    pair[0].wait_recv()
    own = tokv[pl.ds(pl.multiple_of(d * mine, mine), mine), pl.ds(pl.multiple_of(slot * cols, cols), cols)]
    here = (t // per == d).astype(jnp.float32)
    near[...] = (own.astype(jnp.float32) * here + near[...].astype(jnp.float32) * (1.0 - here)).astype(jnp.bfloat16)

    forward = remote(outw, outw, send.at[9], recv.at[9], t, 1 - d)

    @pl.when(t // per == d)
    def _():
        for k in range(1, tp):
            source = lax.rem(t + k, tp)
            remote(outw.at[source], outw.at[source], a2a_send.at[0], a2a_recv.at[source], t, 1 - d).wait_recv()
        pltpu.make_async_copy(outw.at[t], outw.at[t], a2a_send.at[slot]).wait()
        forward.start()

    for c in range(per):
        @pl.when(d * per + c != t)
        def _(c=c):
            spread(c).wait_send()

    @pl.when(t // per == d)
    def _():
        forward.wait_send()

    @pl.when(t // per != d)
    def _():
        forward.wait_recv()

    for op in pair[1:]:
        op.wait_recv()
    for op in pair:
        op.wait_send()
    swap.wait_send()
    for i in range(6):
        loads[2 + 2 * i].wait()


def state_kernel(proj, base, ggain, state, *rest):
    new, mixed = rest[-2], rest[-1]
    seqs = proj.shape[0]
    lines = state.shape[1] // seqs
    wide = 2 * HEAD

    def piece(i):
        return proj[:, i * HEAD : (i + 1) * HEAD].astype(jnp.float32)

    recept, key, value, decay, rate, gate = [piece(i) for i in range(6)]
    forget = jnp.exp(-jnp.exp(-jax.nn.softplus(-(decay + base[...])) - 0.5))
    scale = lax.rsqrt(jnp.sum(key * key, axis=-1, keepdims=True) + 1.0)
    learned = key * jax.nn.sigmoid(rate)

    def spread(row):
        both = jnp.concatenate([row, row], axis=-1)
        return jnp.broadcast_to(both[:, None, :], (seqs, lines, wide))

    def iota(shape, axis):
        return lax.broadcasted_iota(jnp.int32, shape, axis)

    old = state[0].reshape(seqs, lines, wide)
    lane, col = iota((wide, wide), 0), iota((wide, wide), 1)
    same = (lane // HEAD == col // HEAD).astype(jnp.bfloat16)
    odd = ((lane < HEAD) & (lane % 2 == col // HEAD)).astype(jnp.bfloat16)
    turn = (lane // HEAD == col % 2).astype(jnp.bfloat16)
    mask = (iota((lines, wide), 1) % HEAD) // 2 == iota((lines, wide), 0)

    def split(term):
        flat = term.reshape(seqs * lines, wide)
        high = flat.astype(jnp.bfloat16)
        return [high, (flat - high.astype(jnp.float32)).astype(jnp.bfloat16)]

    removed = split(old * spread(key * (-scale * scale)))
    chosen = jnp.where(mask[None], spread(value), 0.0).reshape(seqs * lines, wide).astype(jnp.bfloat16)
    rank = jnp.dot(
        jnp.concatenate(removed + [chosen], axis=1), jnp.concatenate([same, same, odd], axis=0),
        preferred_element_type=jnp.float32,
    ).reshape(seqs, lines, wide)
    updated = old * spread(forget) + rank * spread(learned)
    new[0] = updated.reshape(seqs * lines, wide)
    read = jnp.dot(
        jnp.concatenate(split(updated * spread(recept)), axis=1), jnp.concatenate([turn, turn], axis=0),
        preferred_element_type=jnp.float32,
    ).reshape(seqs, lines, wide)
    read = jnp.sum(jnp.where(mask[None], read, 0.0), axis=1)[:, :HEAD]
    centre = read - jnp.mean(read, axis=-1, keepdims=True)
    normal = centre * lax.rsqrt(jnp.mean(centre * centre, axis=-1, keepdims=True) + group_floor)
    mixed[...] = (normal * ggain[...] * jax.nn.sigmoid(gate)).astype(jnp.bfloat16)


def project_out(lanes, tp, layer, mixed, outw, near, mg, we, send, recv):
    mine, half = mixed.shape[0], mixed.shape[0] // 2
    cols = near.shape[1]
    heads = jnp.concatenate([mixed[0:half, :], mixed[half:mine, :]], axis=1)
    for k in range(2):
        mg[k, lanes.t] = heads[k * half // 2 : (k + 1) * half // 2]
    greet(lanes.peers() + [(lanes.t, 1 - lanes.d)])
    we[...] = jnp.zeros_like(we)
    for k in range(tp):
        block = outw[k, layer]
        we[k * 2 * HEAD : k * 2 * HEAD + HEAD, 0:cols] = block
        we[k * 2 * HEAD + HEAD : (k + 1) * 2 * HEAD, cols : 2 * cols] = block
    gather(lanes, mg, send, recv)
    packed = jnp.concatenate(
        [jnp.concatenate([mg[k, j] for j in range(tp)], axis=1) for k in range(2)], axis=0
    )
    out = jnp.dot(packed, we[...], preferred_element_type=jnp.float32)
    out = jnp.concatenate([out[:, :cols], out[:, cols:]], axis=0)
    return (near[...].astype(jnp.float32) + out).astype(jnp.bfloat16)


def middle_kernel(tp, mixed, outw, near, w1, gain1, proj, after, mg, we, xg, send, recv, xsend, xrecv):
    lanes = Lanes(tp)
    current = project_out(lanes, tp, 0, mixed, outw, near, mg, we, send, recv)
    after[...] = current
    lane = current.shape[1] // 2
    for k in range(2):
        xg[k, lanes.t] = current[:, k * lane : (k + 1) * lane]
    gather(lanes, xg, xsend, xrecv)
    per = tp // 2
    squares, part = 0.0, 0.0
    for e in range(2):
        floats = jnp.concatenate([xg[k, e * per + j] for j in range(per) for k in range(2)], axis=1).astype(jnp.float32)
        squares = squares + jnp.sum(floats * floats, axis=1, keepdims=True)
        normed = (floats * gain1[e, 1:2, :]).astype(jnp.bfloat16)
        part = part + lax.dot_general(normed, w1[e], NT, preferred_element_type=jnp.float32)
    inv = lax.rsqrt(squares / (w1.shape[0] * w1.shape[2]) + norm_floor)
    proj[...] = (inv * part).astype(jnp.bfloat16)


def last_kernel(tp, mixed, outw, near, final, mg, we, xg, xo, send, recv, xsend, xrecv, osend, orecv):
    lanes = Lanes(tp)
    current = project_out(lanes, tp, 1, mixed, outw, near, mg, we, send, recv)
    mine, lane = current.shape[0], current.shape[1] // 2
    d, per = lanes.d, tp // 2
    for k in range(2):
        xg[k, lanes.t] = current[:, k * lane : (k + 1) * lane]
    gather(lanes, xg, xsend, xrecv)
    swap = remote(xg.at[:, pl.ds((1 - d) * per, per)], xo, osend, orecv, lanes.t, 1 - d)
    swap.start()
    for j in range(per):
        for k in range(2):
            at = (2 * j + k) * lane
            final[pl.ds(pl.multiple_of(d * mine, mine), mine), at : at + lane] = xg[k, d * per + j]
    swap.wait()
    for j in range(per):
        for k in range(2):
            at = (2 * j + k) * lane
            final[pl.ds(pl.multiple_of((1 - d) * mine, mine), mine), at : at + lane] = xo[k, j]


def fast(tp, tokens, norm_gain, projections, decay_base, group_gain, output_proj, state):
    rows, feats = tokens.shape
    mine, per = rows // 2, tp // 2
    cols = feats // per
    width = 6 * HEAD
    lines = HEAD * HEAD // (2 * HEAD)
    bf, f32 = jnp.bfloat16, jnp.float32
    shape = jax.ShapeDtypeStruct
    dma = pltpu.SemaphoreType.DMA
    vm, anywhere = pl.BlockSpec(memory_space=pltpu.VMEM), pl.BlockSpec(memory_space=pl.ANY)
    turned = [jnp.swapaxes(w, 1, 2) for w in projections]
    flat = state.reshape(LAYERS, mine * lines, 2 * HEAD)

    def params(number):
        return pltpu.CompilerParams(collective_id=number, has_side_effects=True, vmem_limit_bytes=VMEM_LIMIT)

    proj, near, w1, gain1, outw = pl.pallas_call(
        functools.partial(first_kernel, tp),
        out_shape=(
            shape((mine, width), bf), shape((mine, cols), bf), shape((2, width, feats), bf),
            shape((2, LAYERS, feats), f32), shape((tp, LAYERS, HEAD, cols), bf),
        ),
        in_specs=[anywhere, vm] + [anywhere] * 7,
        out_specs=(vm,) * 5,
        scratch_shapes=[
            pltpu.VMEM((rows, feats), bf), pltpu.VMEM((width, feats), bf), pltpu.VMEM((rows, width + 128), f32),
            pltpu.VMEM((mine, width + 128), f32), dma((13,)), dma((10,)), dma((10,)), dma((per,)), dma((tp,)),
        ],
        compiler_params=params(0),
        name="first",
    )(tokens, norm_gain, *turned, output_proj)

    seqs = min(mine, 32)

    def recur(layer, proj, filled):
        extra = [] if filled is None else [filled]
        return pl.pallas_call(
            state_kernel,
            grid=(mine // seqs,),
            out_shape=(shape(flat.shape, f32), shape((mine, HEAD), bf)),
            in_specs=[
                pl.BlockSpec((seqs, width), lambda i: (i, 0)),
                pl.BlockSpec((1, HEAD), lambda i: (0, 0)),
                pl.BlockSpec((1, HEAD), lambda i: (0, 0)),
                pl.BlockSpec((1, seqs * lines, 2 * HEAD), lambda i: (layer, i, 0)),
            ] + [anywhere] * len(extra),
            out_specs=(
                pl.BlockSpec((1, seqs * lines, 2 * HEAD), lambda i: (layer, i, 0)),
                pl.BlockSpec((seqs, HEAD), lambda i: (i, 0)),
            ),
            input_output_aliases={4: 0} if extra else {},
            compiler_params=pltpu.CompilerParams(vmem_limit_bytes=VMEM_LIMIT),
            name=f"state{layer}",
        )(proj, decay_base[layer : layer + 1], group_gain[layer : layer + 1], flat, *extra)

    filled, mixed = recur(0, proj, None)
    common = [pltpu.VMEM((2, tp, mine // 4, 2 * HEAD), bf), pltpu.VMEM((tp * 2 * HEAD, 2 * cols), bf),
              pltpu.VMEM((2, tp, mine, cols // 2), bf)]
    sems = [dma((2, tp)), dma((2, tp)), dma((2, tp)), dma((2, tp))]
    proj, near = pl.pallas_call(
        functools.partial(middle_kernel, tp),
        out_shape=(shape((mine, width), bf), shape((mine, cols), bf)),
        in_specs=[vm] * 5,
        out_specs=(vm,) * 2,
        scratch_shapes=common + sems,
        compiler_params=params(1),
        name="middle",
    )(mixed, outw, near, w1, gain1)
    filled, mixed = recur(1, proj, filled)
    final = pl.pallas_call(
        functools.partial(last_kernel, tp),
        out_shape=shape((rows, feats), bf),
        in_specs=[vm] * 3,
        out_specs=vm,
        scratch_shapes=common + [pltpu.VMEM((2, per, mine, cols // 2), bf)] + sems + [dma, dma],
        compiler_params=params(2),
        name="last",
    )(mixed, outw, near)
    return (final, filled.reshape(state.shape))


def step(tp, dp, tokens, norm_gain, *rest):
    projections, (decay_base, group_gain, output_proj, state) = rest[:6], rest[6:]
    rows, feats = tokens.shape
    fits = dp == 2 and tp % 8 == 0 and state.shape[2] == 1 and state.shape[1] % 64 == 0 and (feats * dp // tp) % 256 == 0
    if fits:
        return fast(tp, tokens, norm_gain, projections, decay_base, group_gain, output_proj, state)
    return shards(tokens, norm_gain, *rest)


def solution(mesh):
    return jax.shard_map(
        functools.partial(step, mesh.shape["tp"], mesh.shape["dp"]),
        mesh=mesh,
        in_specs=(
            P(None, "dp"),
            P(None, "dp"),
            P(None, "dp", "tp"),
            P(None, "dp", "tp"),
            P(None, "dp", "tp"),
            P(None, "dp", "tp"),
            P(None, "dp", "tp"),
            P(None, "dp", "tp"),
            P(None, "tp"),
            P(None, "tp"),
            P(None, "tp", "dp"),
            P(None, "dp", "tp", None),
        ),
        out_specs=(P(None, "dp"), P(None, "dp", "tp", None)),
        check_vma=False,
    )
```

```python
import functools

import jax
import jax.numpy as jnp
from jax import lax
from jax.experimental import pallas as pl
from jax.experimental.pallas import tpu as pltpu
from jax.sharding import PartitionSpec as P

D = 4096
HEAD = 64
LAYERS = 2


norm_floor = 0.1
group_floor = 0.5


def recurrence(state_block, recept_heads, key_heads, value_heads, decay_heads, rate_heads):
    log_rate = -jax.nn.softplus(-decay_heads) - 0.5
    forget = jnp.exp(-jnp.exp(log_rate))
    learn_rate = jax.nn.sigmoid(rate_heads)
    unit_key = key_heads * lax.rsqrt(jnp.sum(key_heads * key_heads, axis=-1, keepdims=True) + 1.0)
    scaled = key_heads * learn_rate
    removed = jnp.einsum("bhvk,bhk->bhv", state_block, -unit_key, precision=lax.Precision.HIGHEST)
    updated = (
        state_block * forget[:, :, None, :]
        + removed[..., None] * (unit_key * learn_rate)[:, :, None, :]
        + value_heads[..., None] * scaled[:, :, None, :]
    )
    read_out = jnp.einsum("bhvk,bhk->bhv", updated, recept_heads, precision=lax.Precision.HIGHEST)
    centre = read_out - jnp.mean(read_out, axis=-1, keepdims=True)
    normal = centre * lax.rsqrt(jnp.mean(centre * centre, axis=-1, keepdims=True) + group_floor)
    return (updated, normal)


def shards(
    tokens,
    norm_gain,
    receptance,
    key_proj,
    value_proj,
    decay_proj,
    rate_proj,
    gate_proj,
    decay_base,
    group_gain,
    output_proj,
    state,
):
    local_rows = state.shape[1]
    first_row = lax.axis_index("dp") * local_rows
    local_heads = state.shape[2]
    current = tokens
    finals = []
    for section_index in range(LAYERS):
        floats = current.astype(jnp.float32)
        squares = jnp.sum(floats * floats, axis=1)
        normed = (floats * norm_gain[section_index]).astype(jnp.bfloat16)
        part_recept = jnp.dot(normed, receptance[section_index], preferred_element_type=jnp.float32)
        part_key = jnp.dot(normed, key_proj[section_index], preferred_element_type=jnp.float32)
        part_value = jnp.dot(normed, value_proj[section_index], preferred_element_type=jnp.float32)
        part_decay = jnp.dot(normed, decay_proj[section_index], preferred_element_type=jnp.float32)
        part_rate = jnp.dot(normed, rate_proj[section_index], preferred_element_type=jnp.float32)
        part_gate = jnp.dot(normed, gate_proj[section_index], preferred_element_type=jnp.float32)
        totals = lax.psum(squares, "dp")
        own_squares = lax.dynamic_slice_in_dim(totals, first_row, local_rows, 0)
        summed = (
            lax.psum_scatter(part_recept, "dp", scatter_dimension=0, tiled=True),
            lax.psum_scatter(part_key, "dp", scatter_dimension=0, tiled=True),
            lax.psum_scatter(part_value, "dp", scatter_dimension=0, tiled=True),
            lax.psum_scatter(part_decay, "dp", scatter_dimension=0, tiled=True),
            lax.psum_scatter(part_rate, "dp", scatter_dimension=0, tiled=True),
            lax.psum_scatter(part_gate, "dp", scatter_dimension=0, tiled=True),
        )
        inv_rms = lax.rsqrt(own_squares / D + norm_floor)

        def by_head(term):
            rounded = lax.optimization_barrier((inv_rms[:, None] * term).astype(jnp.bfloat16))
            return rounded.astype(jnp.float32).reshape(local_rows, local_heads, HEAD)

        decay_heads = by_head(summed[3]) + decay_base[section_index].reshape(1, local_heads, HEAD)
        updated, normal = recurrence(
            state[section_index].reshape(local_rows, local_heads, HEAD, HEAD),
            by_head(summed[0]),
            by_head(summed[1]),
            by_head(summed[2]),
            decay_heads,
            by_head(summed[4]),
        )
        finals.append(updated.reshape(local_rows, local_heads, HEAD * HEAD))
        gate_value = jax.nn.sigmoid(by_head(summed[5]).reshape(local_rows, local_heads * HEAD))
        mixed_heads = (
            normal.reshape(local_rows, local_heads * HEAD) * group_gain[section_index] * gate_value
        ).astype(jnp.bfloat16)
        weights_out = output_proj[section_index]

        def apply_out(piece, begin, weights_out=weights_out):
            return jnp.dot(piece, weights_out, preferred_element_type=jnp.float32)

        partial_out = apply_out(lax.all_gather(mixed_heads, "dp", axis=0, tiled=True), jnp.int32(0))
        total = lax.psum(partial_out, "tp")
        current = (floats + total).astype(jnp.bfloat16)
    return (current, jnp.stack(finals))


MESH = pl.DeviceIdType.MESH
NT = (((1,), (1,)), ((), ()))
VMEM_LIMIT = 60 * 1024 * 1024


def remote(src, dst, send, recv, t, d):
    return pltpu.make_async_remote_copy(
        src_ref=src, dst_ref=dst, send_sem=send, recv_sem=recv, device_id={"tp": t, "dp": d}, device_id_type=MESH
    )


def greet(peers):
    barrier = pltpu.get_barrier_semaphore()
    for t, d in peers:
        pl.semaphore_signal(barrier, inc=1, device_id={"tp": t, "dp": d}, device_id_type=MESH)
    pl.semaphore_wait(barrier, len(peers))


class Lanes:
    def __init__(self, tp):
        self.t, self.d = lax.axis_index("tp"), lax.axis_index("dp")
        self.nz = tp // 4
        self.x, self.y, self.z = lax.rem(self.t, 2), lax.rem(self.t // 2, 2), self.t // 4

    def at(self, x, y, dz):
        return lax.rem(self.z + dz, self.nz) * 4 + y * 2 + x

    def peers(self):
        near = [self.at(1 - self.x, self.y, 0), self.at(self.x, 1 - self.y, 0)]
        return [(p, self.d) for p in near + [self.at(self.x, self.y, dz) for dz in range(1, self.nz)]]


def gather(lanes, buf, send, recv, beside=None, arrived=None):
    x, y, nz, d = lanes.x, lanes.y, lanes.nz, lanes.d
    xp, yp = lanes.at(1 - x, y, 0), lanes.at(x, 1 - y, 0)
    started = []
    count = [0, 0]

    def put(half, block, target):
        op = remote(buf.at[half, block], buf.at[half, block], send.at[half, count[half]], recv.at[half, block], target, d)
        count[half] += 1
        op.start()
        started.append(op)

    def got(half, block):
        remote(buf.at[half, block], buf.at[half, block], send.at[half, 0], recv.at[half, block], xp, d).wait_recv()
        if arrived is not None:
            arrived(half, block)

    zs = list(range(1, nz))
    own = lanes.t
    put(0, own, yp)
    for dz in zs:
        put(1, own, lanes.at(x, y, dz))
        put(0, own, lanes.at(x, y, dz))
    put(1, own, xp)
    put(1, own, yp)
    put(0, own, xp)
    if beside is not None:
        beside()
    got(0, yp)
    for dz in zs:
        put(0, yp, lanes.at(x, y, dz))
    put(0, yp, xp)
    got(1, xp)
    put(1, xp, yp)
    for dz in zs:
        block = lanes.at(x, y, dz)
        got(1, block)
        put(1, block, xp)
        put(1, block, yp)
        got(0, block)
        put(0, block, xp)
    for dz in zs:
        block = lanes.at(x, 1 - y, dz)
        got(0, block)
        put(0, block, xp)
        block = lanes.at(1 - x, y, dz)
        got(1, block)
        put(1, block, yp)
    for dz in range(nz):
        for k in range(2):
            got(0, lanes.at(1 - x, k, dz))
            got(1, lanes.at(k, 1 - y, dz))
    for op in started:
        op.wait_send()


def first_kernel(
    tp, tok, gain, wr, wk, wv, wd, wa, wg, wo, proj, near, w1, gain1, outw,
    tokv, w0, part, inbox, load, send, recv, a2a_send, a2a_recv, on_send, on_recv,
):
    lanes = Lanes(tp)
    t, d = lanes.t, lanes.d
    per = tp // 2
    rows, feats = tok.shape
    mine = rows // 2
    cols = feats // per
    weights = (wr, wk, wv, wd, wa, wg)
    loads = [pltpu.make_async_copy(tok, tokv, load.at[0])]
    for i, w in enumerate(weights):
        loads.append(pltpu.make_async_copy(w.at[0], w0.at[pl.ds(i * HEAD, HEAD)], load.at[1 + i]))
        loads.append(pltpu.make_async_copy(w.at[1], w1.at[d, pl.ds(i * HEAD, HEAD)], load.at[7 + i]))
    for op in loads:
        op.start()
    greet([(lax.rem(t + k, tp), d) for k in range(1, tp)] + [(t, 1 - d)])

    def spread(c):
        target = d * per + c
        return remote(wo.at[:, :, pl.ds(c * cols, cols)], outw.at[t], a2a_send.at[c], a2a_recv.at[t], target, d)

    for c in range(per):
        @pl.when(d * per + c != t)
        def _(c=c):
            spread(c).start()

        @pl.when(d * per + c == t)
        def _(c=c):
            pltpu.make_async_copy(wo.at[:, :, pl.ds(c * cols, cols)], outw.at[t], a2a_send.at[c]).start()

    loads[0].wait()
    slot = lax.rem(t, per)
    there = (1 - d) * mine
    pair = [
        remote(
            tokv.at[pl.ds(pl.multiple_of(there, mine), mine), pl.ds(pl.multiple_of(slot * cols, cols), cols)],
            near, send.at[0], recv.at[0], t, 1 - d,
        ),
        remote(gain, gain1.at[d], send.at[1], recv.at[1], t, 1 - d),
    ]
    for i, w in enumerate(weights):
        pair.append(remote(w.at[1], w1.at[d, pl.ds(i * HEAD, HEAD)], send.at[2 + i], recv.at[2 + i], t, 1 - d))
    pair[0].start()
    pair[1].start()
    gain1[pl.ds(d, 1)] = gain[...][None]

    floats = tokv[...].astype(jnp.float32)
    squares = jnp.sum(floats * floats, axis=1, keepdims=True)
    normed = (floats * gain[0:1, :]).astype(jnp.bfloat16)
    for i in range(6):
        loads[1 + 2 * i].wait()
    width = 6 * HEAD
    part[:, 0:width] = lax.dot_general(normed, w0[...], NT, preferred_element_type=jnp.float32)
    part[:, width:] = jnp.broadcast_to(squares, (rows, part.shape[1] - width))
    swap = remote(part.at[pl.ds(pl.multiple_of(there, mine), mine)], inbox, send.at[8], recv.at[8], t, 1 - d)
    swap.start()
    for op in pair[2:]:
        op.start()
    swap.wait_recv()
    total = part[pl.ds(pl.multiple_of(d * mine, mine), mine), :] + inbox[...]
    inv = lax.rsqrt(total[:, width : width + 1] / (feats * 2) + norm_floor)
    proj[...] = (inv * total[:, :width]).astype(jnp.bfloat16)

    pair[0].wait_recv()
    own = tokv[pl.ds(pl.multiple_of(d * mine, mine), mine), pl.ds(pl.multiple_of(slot * cols, cols), cols)]
    here = (t // per == d).astype(jnp.float32)
    near[...] = (own.astype(jnp.float32) * here + near[...].astype(jnp.float32) * (1.0 - here)).astype(jnp.bfloat16)

    def forward(source):
        return remote(outw.at[source], outw.at[source], on_send.at[source], on_recv.at[source], t, 1 - d)

    @pl.when(t // per == d)
    def _():
        pltpu.make_async_copy(outw.at[t], outw.at[t], a2a_send.at[slot]).wait()
        forward(t).start()
        for k in range(1, tp):
            source = lax.rem(t + k, tp)
            remote(outw.at[source], outw.at[source], a2a_send.at[0], a2a_recv.at[source], t, 1 - d).wait_recv()
            forward(source).start()

    for c in range(per):
        @pl.when(d * per + c != t)
        def _(c=c):
            spread(c).wait_send()

    @pl.when(t // per == d)
    def _():
        for k in range(tp):
            forward(k).wait_send()

    @pl.when(t // per != d)
    def _():
        for k in range(tp):
            forward(k).wait_recv()

    for op in pair[1:]:
        op.wait_recv()
    for op in pair:
        op.wait_send()
    swap.wait_send()
    for i in range(6):
        loads[2 + 2 * i].wait()


def state_kernel(proj, base, ggain, state, *rest):
    new, mixed = rest[-2], rest[-1]
    seqs = proj.shape[0]
    lines = state.shape[1] // seqs
    wide = 2 * HEAD

    def piece(i):
        return proj[:, i * HEAD : (i + 1) * HEAD].astype(jnp.float32)

    recept, key, value, decay, rate, gate = [piece(i) for i in range(6)]
    forget = jnp.exp(-jnp.exp(-jax.nn.softplus(-(decay + base[...])) - 0.5))
    scale = lax.rsqrt(jnp.sum(key * key, axis=-1, keepdims=True) + 1.0)
    learned = key * jax.nn.sigmoid(rate)

    def spread(row):
        both = jnp.concatenate([row, row], axis=-1)
        return jnp.broadcast_to(both[:, None, :], (seqs, lines, wide))

    def iota(shape, axis):
        return lax.broadcasted_iota(jnp.int32, shape, axis)

    old = state[0].reshape(seqs, lines, wide)
    lane, col = iota((wide, wide), 0), iota((wide, wide), 1)
    same = (lane // HEAD == col // HEAD).astype(jnp.bfloat16)
    odd = ((lane < HEAD) & (lane % 2 == col // HEAD)).astype(jnp.bfloat16)
    turn = (lane // HEAD == col % 2).astype(jnp.bfloat16)
    mask = (iota((lines, wide), 1) % HEAD) // 2 == iota((lines, wide), 0)

    def split(term):
        flat = term.reshape(seqs * lines, wide)
        high = flat.astype(jnp.bfloat16)
        return [high, (flat - high.astype(jnp.float32)).astype(jnp.bfloat16)]

    removed = split(old * spread(key * (-scale * scale)))
    chosen = jnp.where(mask[None], spread(value), 0.0).reshape(seqs * lines, wide).astype(jnp.bfloat16)
    rank = jnp.dot(
        jnp.concatenate(removed + [chosen], axis=1), jnp.concatenate([same, same, odd], axis=0),
        preferred_element_type=jnp.float32,
    ).reshape(seqs, lines, wide)
    updated = old * spread(forget) + rank * spread(learned)
    new[0] = updated.reshape(seqs * lines, wide)
    read = jnp.dot(
        jnp.concatenate(split(updated * spread(recept)), axis=1), jnp.concatenate([turn, turn], axis=0),
        preferred_element_type=jnp.float32,
    ).reshape(seqs, lines, wide)
    read = jnp.sum(jnp.where(mask[None], read, 0.0), axis=1)[:, :HEAD]
    centre = read - jnp.mean(read, axis=-1, keepdims=True)
    normal = centre * lax.rsqrt(jnp.mean(centre * centre, axis=-1, keepdims=True) + group_floor)
    mixed[...] = (normal * ggain[...] * jax.nn.sigmoid(gate)).astype(jnp.bfloat16)


def project_out(lanes, tp, layer, mixed, outw, near, mg, we, send, recv):
    mine, half = mixed.shape[0], mixed.shape[0] // 2
    cols = near.shape[1]
    heads = jnp.concatenate([mixed[0:half, :], mixed[half:mine, :]], axis=1)
    for k in range(2):
        mg[k, lanes.t] = heads[k * half // 2 : (k + 1) * half // 2]
    greet(lanes.peers() + [(lanes.t, 1 - lanes.d)])

    def place():
        zero = jnp.zeros((HEAD, cols), we.dtype)
        for k in range(tp):
            block = outw[k, layer]
            top, bottom = pl.ds(k * 2 * HEAD, HEAD), pl.ds(k * 2 * HEAD + HEAD, HEAD)
            we[top, 0:cols] = block
            we[top, cols : 2 * cols] = zero
            we[bottom, 0:cols] = zero
            we[bottom, cols : 2 * cols] = block

    gather(lanes, mg, send, recv, beside=place)
    packed = jnp.concatenate(
        [jnp.concatenate([mg[k, j] for j in range(tp)], axis=1) for k in range(2)], axis=0
    )
    out = jnp.dot(packed, we[...], preferred_element_type=jnp.float32)
    out = jnp.concatenate([out[:, :cols], out[:, cols:]], axis=0)
    return (near[...].astype(jnp.float32) + out).astype(jnp.bfloat16)


def middle_kernel(tp, mixed, outw, near, w1, gain1, proj, after, mg, we, xg, send, recv, xsend, xrecv, w1v, wsem):
    lanes = Lanes(tp)
    load = pltpu.make_async_copy(w1, w1v, wsem)
    load.start()
    current = project_out(lanes, tp, 0, mixed, outw, near, mg, we, send, recv)
    after[...] = current
    lane = current.shape[1] // 2
    for k in range(2):
        xg[k, lanes.t] = current[:, k * lane : (k + 1) * lane]
    gather(lanes, xg, xsend, xrecv)
    per = tp // 2
    load.wait()
    squares, part = 0.0, 0.0
    for e in range(2):
        floats = jnp.concatenate([xg[k, e * per + j] for j in range(per) for k in range(2)], axis=1).astype(jnp.float32)
        squares = squares + jnp.sum(floats * floats, axis=1, keepdims=True)
        normed = (floats * gain1[e, 1:2, :]).astype(jnp.bfloat16)
        part = part + lax.dot_general(normed, w1v[e], NT, preferred_element_type=jnp.float32)
    inv = lax.rsqrt(squares / (w1.shape[0] * w1.shape[2]) + norm_floor)
    proj[...] = (inv * part).astype(jnp.bfloat16)


def last_kernel(tp, mixed, outw, near, final, mg, we, xg, xo, send, recv, xsend, xrecv, osend, orecv):
    lanes = Lanes(tp)
    current = project_out(lanes, tp, 1, mixed, outw, near, mg, we, send, recv)
    mine, lane = current.shape[0], current.shape[1] // 2
    d, per = lanes.d, tp // 2
    for k in range(2):
        xg[k, lanes.t] = current[:, k * lane : (k + 1) * lane]

    def hand(half, block):
        place = lax.rem(block, per)
        return remote(xg.at[half, block], xo.at[half, place], osend.at[half, place], orecv.at[half, place], lanes.t, 1 - d)

    def arrived(half, block):
        @pl.when(block // per == 1 - d)
        def _():
            hand(half, block).start()

    arrived(0, lanes.t)
    arrived(1, lanes.t)
    gather(lanes, xg, xsend, xrecv, arrived=arrived)
    for j in range(per):
        for k in range(2):
            at = (2 * j + k) * lane
            final[pl.ds(pl.multiple_of(d * mine, mine), mine), at : at + lane] = xg[k, d * per + j]
    for j in range(per):
        for k in range(2):
            hand(k, (1 - d) * per + j).wait_recv()
    for j in range(per):
        for k in range(2):
            at = (2 * j + k) * lane
            final[pl.ds(pl.multiple_of((1 - d) * mine, mine), mine), at : at + lane] = xo[k, j]
    for j in range(per):
        for k in range(2):
            hand(k, (1 - d) * per + j).wait_send()


def fast(tp, tokens, norm_gain, projections, decay_base, group_gain, output_proj, state):
    rows, feats = tokens.shape
    mine, per = rows // 2, tp // 2
    cols = feats // per
    width = 6 * HEAD
    lines = HEAD * HEAD // (2 * HEAD)
    bf, f32 = jnp.bfloat16, jnp.float32
    shape = jax.ShapeDtypeStruct
    dma = pltpu.SemaphoreType.DMA
    vm, anywhere = pl.BlockSpec(memory_space=pltpu.VMEM), pl.BlockSpec(memory_space=pl.ANY)
    turned = [jnp.swapaxes(w, 1, 2) for w in projections]
    flat = state.reshape(LAYERS, mine * lines, 2 * HEAD)

    def params(number):
        return pltpu.CompilerParams(collective_id=number, has_side_effects=True, vmem_limit_bytes=VMEM_LIMIT)

    proj, near, w1, gain1, outw = pl.pallas_call(
        functools.partial(first_kernel, tp),
        out_shape=(
            shape((mine, width), bf), shape((mine, cols), bf), shape((2, width, feats), bf),
            shape((2, LAYERS, feats), f32), shape((tp, LAYERS, HEAD, cols), bf),
        ),
        in_specs=[anywhere, vm] + [anywhere] * 7,
        out_specs=(vm,) * 5,
        scratch_shapes=[
            pltpu.VMEM((rows, feats), bf), pltpu.VMEM((width, feats), bf), pltpu.VMEM((rows, width + 128), f32),
            pltpu.VMEM((mine, width + 128), f32), dma((13,)), dma((9,)), dma((9,)), dma((per,)), dma((tp,)),
            dma((tp,)), dma((tp,)),
        ],
        compiler_params=params(0),
        name="first",
    )(tokens, norm_gain, *turned, output_proj)

    seqs = min(mine, 32)

    def recur(layer, proj, filled):
        extra = [] if filled is None else [filled]
        return pl.pallas_call(
            state_kernel,
            grid=(mine // seqs,),
            out_shape=(shape(flat.shape, f32), shape((mine, HEAD), bf)),
            in_specs=[
                pl.BlockSpec((seqs, width), lambda i: (i, 0)),
                pl.BlockSpec((1, HEAD), lambda i: (0, 0)),
                pl.BlockSpec((1, HEAD), lambda i: (0, 0)),
                pl.BlockSpec((1, seqs * lines, 2 * HEAD), lambda i: (layer, i, 0)),
            ] + [anywhere] * len(extra),
            out_specs=(
                pl.BlockSpec((1, seqs * lines, 2 * HEAD), lambda i: (layer, i, 0)),
                pl.BlockSpec((seqs, HEAD), lambda i: (i, 0)),
            ),
            input_output_aliases={4: 0} if extra else {},
            compiler_params=pltpu.CompilerParams(vmem_limit_bytes=VMEM_LIMIT),
            name=f"state{layer}",
        )(proj, decay_base[layer : layer + 1], group_gain[layer : layer + 1], flat, *extra)

    filled, mixed = recur(0, proj, None)
    common = [pltpu.VMEM((2, tp, mine // 4, 2 * HEAD), bf), pltpu.VMEM((tp * 2 * HEAD, 2 * cols), bf),
              pltpu.VMEM((2, tp, mine, cols // 2), bf)]
    sems = [dma((2, tp)), dma((2, tp)), dma((2, tp)), dma((2, tp))]
    proj, near = pl.pallas_call(
        functools.partial(middle_kernel, tp),
        out_shape=(shape((mine, width), bf), shape((mine, cols), bf)),
        in_specs=[vm] * 3 + [anywhere, vm],
        out_specs=(vm,) * 2,
        scratch_shapes=common + sems + [pltpu.VMEM(w1.shape, bf), dma],
        compiler_params=params(1),
        name="middle",
    )(mixed, outw, near, w1, gain1)
    filled, mixed = recur(1, proj, filled)
    final = pl.pallas_call(
        functools.partial(last_kernel, tp),
        out_shape=shape((rows, feats), bf),
        in_specs=[vm] * 3,
        out_specs=vm,
        scratch_shapes=common + [pltpu.VMEM((2, per, mine, cols // 2), bf)] + sems + [dma((2, per)), dma((2, per))],
        compiler_params=params(2),
        name="last",
    )(mixed, outw, near)
    return (final, filled.reshape(state.shape))


def step(tp, dp, tokens, norm_gain, *rest):
    projections, (decay_base, group_gain, output_proj, state) = rest[:6], rest[6:]
    rows, feats = tokens.shape
    fits = dp == 2 and tp % 8 == 0 and state.shape[2] == 1 and state.shape[1] % 64 == 0 and (feats * dp // tp) % 256 == 0
    if fits:
        return fast(tp, tokens, norm_gain, projections, decay_base, group_gain, output_proj, state)
    return shards(tokens, norm_gain, *rest)


def solution(mesh):
    return jax.shard_map(
        functools.partial(step, mesh.shape["tp"], mesh.shape["dp"]),
        mesh=mesh,
        in_specs=(
            P(None, "dp"),
            P(None, "dp"),
            P(None, "dp", "tp"),
            P(None, "dp", "tp"),
            P(None, "dp", "tp"),
            P(None, "dp", "tp"),
            P(None, "dp", "tp"),
            P(None, "dp", "tp"),
            P(None, "tp"),
            P(None, "tp"),
            P(None, "tp", "dp"),
            P(None, "dp", "tp", None),
        ),
        out_specs=(P(None, "dp"), P(None, "dp", "tp", None)),
        check_vma=False,
    )
```

```python
import functools

import jax
import jax.numpy as jnp
from jax import lax
from jax.experimental import pallas as pl
from jax.experimental.pallas import tpu as pltpu
from jax.sharding import PartitionSpec as P

D = 4096
HEAD = 64
LAYERS = 2


norm_floor = 0.1
group_floor = 0.5


def recurrence(state_block, recept_heads, key_heads, value_heads, decay_heads, rate_heads):
    log_rate = -jax.nn.softplus(-decay_heads) - 0.5
    forget = jnp.exp(-jnp.exp(log_rate))
    learn_rate = jax.nn.sigmoid(rate_heads)
    unit_key = key_heads * lax.rsqrt(jnp.sum(key_heads * key_heads, axis=-1, keepdims=True) + 1.0)
    scaled = key_heads * learn_rate
    removed = jnp.einsum("bhvk,bhk->bhv", state_block, -unit_key, precision=lax.Precision.HIGHEST)
    updated = (
        state_block * forget[:, :, None, :]
        + removed[..., None] * (unit_key * learn_rate)[:, :, None, :]
        + value_heads[..., None] * scaled[:, :, None, :]
    )
    read_out = jnp.einsum("bhvk,bhk->bhv", updated, recept_heads, precision=lax.Precision.HIGHEST)
    centre = read_out - jnp.mean(read_out, axis=-1, keepdims=True)
    normal = centre * lax.rsqrt(jnp.mean(centre * centre, axis=-1, keepdims=True) + group_floor)
    return (updated, normal)


def shards(
    tokens,
    norm_gain,
    receptance,
    key_proj,
    value_proj,
    decay_proj,
    rate_proj,
    gate_proj,
    decay_base,
    group_gain,
    output_proj,
    state,
):
    local_rows = state.shape[1]
    first_row = lax.axis_index("dp") * local_rows
    local_heads = state.shape[2]
    current = tokens
    finals = []
    for section_index in range(LAYERS):
        floats = current.astype(jnp.float32)
        squares = jnp.sum(floats * floats, axis=1)
        normed = (floats * norm_gain[section_index]).astype(jnp.bfloat16)
        part_recept = jnp.dot(normed, receptance[section_index], preferred_element_type=jnp.float32)
        part_key = jnp.dot(normed, key_proj[section_index], preferred_element_type=jnp.float32)
        part_value = jnp.dot(normed, value_proj[section_index], preferred_element_type=jnp.float32)
        part_decay = jnp.dot(normed, decay_proj[section_index], preferred_element_type=jnp.float32)
        part_rate = jnp.dot(normed, rate_proj[section_index], preferred_element_type=jnp.float32)
        part_gate = jnp.dot(normed, gate_proj[section_index], preferred_element_type=jnp.float32)
        totals = lax.psum(squares, "dp")
        own_squares = lax.dynamic_slice_in_dim(totals, first_row, local_rows, 0)
        summed = (
            lax.psum_scatter(part_recept, "dp", scatter_dimension=0, tiled=True),
            lax.psum_scatter(part_key, "dp", scatter_dimension=0, tiled=True),
            lax.psum_scatter(part_value, "dp", scatter_dimension=0, tiled=True),
            lax.psum_scatter(part_decay, "dp", scatter_dimension=0, tiled=True),
            lax.psum_scatter(part_rate, "dp", scatter_dimension=0, tiled=True),
            lax.psum_scatter(part_gate, "dp", scatter_dimension=0, tiled=True),
        )
        inv_rms = lax.rsqrt(own_squares / D + norm_floor)

        def by_head(term):
            rounded = lax.optimization_barrier((inv_rms[:, None] * term).astype(jnp.bfloat16))
            return rounded.astype(jnp.float32).reshape(local_rows, local_heads, HEAD)

        decay_heads = by_head(summed[3]) + decay_base[section_index].reshape(1, local_heads, HEAD)
        updated, normal = recurrence(
            state[section_index].reshape(local_rows, local_heads, HEAD, HEAD),
            by_head(summed[0]),
            by_head(summed[1]),
            by_head(summed[2]),
            decay_heads,
            by_head(summed[4]),
        )
        finals.append(updated.reshape(local_rows, local_heads, HEAD * HEAD))
        gate_value = jax.nn.sigmoid(by_head(summed[5]).reshape(local_rows, local_heads * HEAD))
        mixed_heads = (
            normal.reshape(local_rows, local_heads * HEAD) * group_gain[section_index] * gate_value
        ).astype(jnp.bfloat16)
        weights_out = output_proj[section_index]

        def apply_out(piece, begin, weights_out=weights_out):
            return jnp.dot(piece, weights_out, preferred_element_type=jnp.float32)

        partial_out = apply_out(lax.all_gather(mixed_heads, "dp", axis=0, tiled=True), jnp.int32(0))
        total = lax.psum(partial_out, "tp")
        current = (floats + total).astype(jnp.bfloat16)
    return (current, jnp.stack(finals))


MESH = pl.DeviceIdType.MESH
NT = (((1,), (1,)), ((), ()))
VMEM_LIMIT = 60 * 1024 * 1024


def remote(src, dst, send, recv, t, d):
    return pltpu.make_async_remote_copy(
        src_ref=src, dst_ref=dst, send_sem=send, recv_sem=recv, device_id={"tp": t, "dp": d}, device_id_type=MESH
    )


def greet(peers):
    barrier = pltpu.get_barrier_semaphore()
    for t, d in peers:
        pl.semaphore_signal(barrier, inc=1, device_id={"tp": t, "dp": d}, device_id_type=MESH)
    pl.semaphore_wait(barrier, len(peers))


class Lanes:
    def __init__(self, tp):
        self.t, self.d = lax.axis_index("tp"), lax.axis_index("dp")
        self.nz = tp // 4
        self.x, self.y, self.z = lax.rem(self.t, 2), lax.rem(self.t // 2, 2), self.t // 4

    def at(self, x, y, dz):
        return lax.rem(self.z + dz, self.nz) * 4 + y * 2 + x

    def peers(self):
        near = [self.at(1 - self.x, self.y, 0), self.at(self.x, 1 - self.y, 0)]
        return [(p, self.d) for p in near + [self.at(self.x, self.y, dz) for dz in range(1, self.nz)]]


def gather(lanes, buf, send, recv, beside=None, arrived=None):
    x, y, nz, d = lanes.x, lanes.y, lanes.nz, lanes.d
    xp, yp = lanes.at(1 - x, y, 0), lanes.at(x, 1 - y, 0)
    started = []
    count = [0, 0]

    def put(half, block, target):
        op = remote(buf.at[half, block], buf.at[half, block], send.at[half, count[half]], recv.at[half, block], target, d)
        count[half] += 1
        op.start()
        started.append(op)

    def got(half, block):
        remote(buf.at[half, block], buf.at[half, block], send.at[half, 0], recv.at[half, block], xp, d).wait_recv()
        if arrived is not None:
            arrived(half, block)

    zs = list(range(1, nz))
    own = lanes.t
    put(0, own, yp)
    for dz in zs:
        put(1, own, lanes.at(x, y, dz))
        put(0, own, lanes.at(x, y, dz))
    put(1, own, xp)
    put(1, own, yp)
    put(0, own, xp)
    if beside is not None:
        beside()
    got(0, yp)
    for dz in zs:
        put(0, yp, lanes.at(x, y, dz))
    put(0, yp, xp)
    got(1, xp)
    put(1, xp, yp)
    for dz in zs:
        block = lanes.at(x, y, dz)
        got(1, block)
        put(1, block, xp)
        put(1, block, yp)
        got(0, block)
        put(0, block, xp)
    for dz in zs:
        block = lanes.at(x, 1 - y, dz)
        got(0, block)
        put(0, block, xp)
        block = lanes.at(1 - x, y, dz)
        got(1, block)
        put(1, block, yp)
    for dz in range(nz):
        for k in range(2):
            got(0, lanes.at(1 - x, k, dz))
            got(1, lanes.at(k, 1 - y, dz))
    for op in started:
        op.wait_send()


def first_kernel(
    tp, tok, gain, wr, wk, wv, wd, wa, wg, wo, proj, near, w1, gain1, outw,
    tokv, w0, part, inbox, load, send, recv, a2a_send, a2a_recv, on_send, on_recv,
):
    lanes = Lanes(tp)
    t, d = lanes.t, lanes.d
    per = tp // 2
    rows, feats = tok.shape
    mine = rows // 2
    cols = feats // per
    weights = (wr, wk, wv, wd, wa, wg)
    loads = [pltpu.make_async_copy(tok, tokv, load.at[0])]
    for i, w in enumerate(weights):
        loads.append(pltpu.make_async_copy(w.at[0], w0.at[pl.ds(i * HEAD, HEAD)], load.at[1 + i]))
        loads.append(pltpu.make_async_copy(w.at[1], w1.at[d, pl.ds(i * HEAD, HEAD)], load.at[7 + i]))
    for op in loads:
        op.start()
    greet([(lax.rem(t + k, tp), d) for k in range(1, tp)] + [(t, 1 - d)])

    def spread(c):
        target = d * per + c
        return remote(wo.at[:, :, pl.ds(pl.multiple_of(c * cols, cols), cols)], outw.at[t], a2a_send.at[c], a2a_recv.at[t], target, d)

    for k in range(per):
        c = lax.rem(t + k, per)

        @pl.when(d * per + c != t)
        def _(c=c):
            spread(c).start()

        @pl.when(d * per + c == t)
        def _(c=c):
            pltpu.make_async_copy(wo.at[:, :, pl.ds(pl.multiple_of(c * cols, cols), cols)], outw.at[t], a2a_send.at[c]).start()

    loads[0].wait()
    slot = lax.rem(t, per)
    there = (1 - d) * mine
    pair = [
        remote(
            tokv.at[pl.ds(pl.multiple_of(there, mine), mine), pl.ds(pl.multiple_of(slot * cols, cols), cols)],
            near, send.at[0], recv.at[0], t, 1 - d,
        ),
        remote(gain, gain1.at[d], send.at[1], recv.at[1], t, 1 - d),
    ]
    for i, w in enumerate(weights):
        pair.append(remote(w.at[1], w1.at[d, pl.ds(i * HEAD, HEAD)], send.at[2 + i], recv.at[2 + i], t, 1 - d))
    pair[0].start()
    pair[1].start()
    gain1[pl.ds(d, 1)] = gain[...][None]

    floats = tokv[...].astype(jnp.float32)
    squares = jnp.sum(floats * floats, axis=1, keepdims=True)
    normed = (floats * gain[0:1, :]).astype(jnp.bfloat16)
    for i in range(6):
        loads[1 + 2 * i].wait()
    width = 6 * HEAD
    part[:, 0:width] = lax.dot_general(normed, w0[...], NT, preferred_element_type=jnp.float32)
    part[:, width:] = jnp.broadcast_to(squares, (rows, part.shape[1] - width))
    swap = remote(part.at[pl.ds(pl.multiple_of(there, mine), mine)], inbox, send.at[8], recv.at[8], t, 1 - d)
    swap.start()
    for op in pair[2:]:
        op.start()
    swap.wait_recv()
    total = part[pl.ds(pl.multiple_of(d * mine, mine), mine), :] + inbox[...]
    inv = lax.rsqrt(total[:, width : width + 1] / (feats * 2) + norm_floor)
    proj[...] = (inv * total[:, :width]).astype(jnp.bfloat16)

    pair[0].wait_recv()
    own = tokv[pl.ds(pl.multiple_of(d * mine, mine), mine), pl.ds(pl.multiple_of(slot * cols, cols), cols)]
    here = (t // per == d).astype(jnp.float32)
    near[...] = (own.astype(jnp.float32) * here + near[...].astype(jnp.float32) * (1.0 - here)).astype(jnp.bfloat16)

    def forward(source):
        return remote(outw.at[source], outw.at[source], on_send.at[source], on_recv.at[source], t, 1 - d)

    @pl.when(t // per == d)
    def _():
        pltpu.make_async_copy(outw.at[t], outw.at[t], a2a_send.at[slot]).wait()
        forward(t).start()
        for k in range(1, tp):
            source = lax.rem(t + k, tp)
            remote(outw.at[source], outw.at[source], a2a_send.at[0], a2a_recv.at[source], t, 1 - d).wait_recv()
            forward(source).start()

    for c in range(per):
        @pl.when(d * per + c != t)
        def _(c=c):
            spread(c).wait_send()

    @pl.when(t // per == d)
    def _():
        for k in range(tp):
            forward(k).wait_send()

    @pl.when(t // per != d)
    def _():
        for k in range(tp):
            forward(k).wait_recv()

    for op in pair[1:]:
        op.wait_recv()
    for op in pair:
        op.wait_send()
    swap.wait_send()
    for i in range(6):
        loads[2 + 2 * i].wait()


def state_kernel(proj, base, ggain, state, *rest):
    new, mixed = rest[-2], rest[-1]
    seqs = proj.shape[0]
    lines = state.shape[1] // seqs
    wide = 2 * HEAD

    def piece(i):
        return proj[:, i * HEAD : (i + 1) * HEAD].astype(jnp.float32)

    recept, key, value, decay, rate, gate = [piece(i) for i in range(6)]
    forget = jnp.exp(-jnp.exp(-jax.nn.softplus(-(decay + base[...])) - 0.5))
    scale = lax.rsqrt(jnp.sum(key * key, axis=-1, keepdims=True) + 1.0)
    learned = key * jax.nn.sigmoid(rate)

    def spread(row):
        both = jnp.concatenate([row, row], axis=-1)
        return jnp.broadcast_to(both[:, None, :], (seqs, lines, wide))

    def iota(shape, axis):
        return lax.broadcasted_iota(jnp.int32, shape, axis)

    old = state[0].reshape(seqs, lines, wide)
    lane, col = iota((wide, wide), 0), iota((wide, wide), 1)
    same = (lane // HEAD == col // HEAD).astype(jnp.bfloat16)
    odd = ((lane < HEAD) & (lane % 2 == col // HEAD)).astype(jnp.bfloat16)
    turn = (lane // HEAD == col % 2).astype(jnp.bfloat16)
    mask = (iota((lines, wide), 1) % HEAD) // 2 == iota((lines, wide), 0)

    def split(term):
        flat = term.reshape(seqs * lines, wide)
        high = flat.astype(jnp.bfloat16)
        return [high, (flat - high.astype(jnp.float32)).astype(jnp.bfloat16)]

    removed = split(old * spread(key * (-scale * scale)))
    chosen = jnp.where(mask[None], spread(value), 0.0).reshape(seqs * lines, wide).astype(jnp.bfloat16)
    rank = jnp.dot(
        jnp.concatenate(removed + [chosen], axis=1), jnp.concatenate([same, same, odd], axis=0),
        preferred_element_type=jnp.float32,
    ).reshape(seqs, lines, wide)
    updated = old * spread(forget) + rank * spread(learned)
    new[0] = updated.reshape(seqs * lines, wide)
    read = jnp.dot(
        jnp.concatenate(split(updated * spread(recept)), axis=1), jnp.concatenate([turn, turn], axis=0),
        preferred_element_type=jnp.float32,
    ).reshape(seqs, lines, wide)
    read = jnp.sum(jnp.where(mask[None], read, 0.0), axis=1)[:, :HEAD]
    centre = read - jnp.mean(read, axis=-1, keepdims=True)
    normal = centre * lax.rsqrt(jnp.mean(centre * centre, axis=-1, keepdims=True) + group_floor)
    mixed[...] = (normal * ggain[...] * jax.nn.sigmoid(gate)).astype(jnp.bfloat16)


def project_out(lanes, tp, layer, mixed, outw, near, mg, we, send, recv):
    mine, half = mixed.shape[0], mixed.shape[0] // 2
    cols = near.shape[1]
    heads = jnp.concatenate([mixed[0:half, :], mixed[half:mine, :]], axis=1)
    for k in range(2):
        mg[k, lanes.t] = heads[k * half // 2 : (k + 1) * half // 2]
    greet(lanes.peers() + [(lanes.t, 1 - lanes.d)])

    def place():
        zero = jnp.zeros((HEAD, cols), we.dtype)
        for k in range(tp):
            block = outw[k, layer]
            top, bottom = pl.ds(k * 2 * HEAD, HEAD), pl.ds(k * 2 * HEAD + HEAD, HEAD)
            we[top, 0:cols] = block
            we[top, cols : 2 * cols] = zero
            we[bottom, 0:cols] = zero
            we[bottom, cols : 2 * cols] = block

    gather(lanes, mg, send, recv, beside=place)
    packed = jnp.concatenate(
        [jnp.concatenate([mg[k, j] for j in range(tp)], axis=1) for k in range(2)], axis=0
    )
    out = jnp.dot(packed, we[...], preferred_element_type=jnp.float32)
    out = jnp.concatenate([out[:, :cols], out[:, cols:]], axis=0)
    return (near[...].astype(jnp.float32) + out).astype(jnp.bfloat16)


def middle_kernel(tp, mixed, outw, near, w1, gain1, proj, after, mg, we, xg, send, recv, xsend, xrecv, w1v, wsem):
    lanes = Lanes(tp)
    load = pltpu.make_async_copy(w1, w1v, wsem)
    load.start()
    current = project_out(lanes, tp, 0, mixed, outw, near, mg, we, send, recv)
    after[...] = current
    lane = current.shape[1] // 2
    for k in range(2):
        xg[k, lanes.t] = current[:, k * lane : (k + 1) * lane]
    gather(lanes, xg, xsend, xrecv)
    per = tp // 2
    load.wait()
    squares, part = 0.0, 0.0
    for e in range(2):
        floats = jnp.concatenate([xg[k, e * per + j] for j in range(per) for k in range(2)], axis=1).astype(jnp.float32)
        squares = squares + jnp.sum(floats * floats, axis=1, keepdims=True)
        normed = (floats * gain1[e, 1:2, :]).astype(jnp.bfloat16)
        part = part + lax.dot_general(normed, w1v[e], NT, preferred_element_type=jnp.float32)
    inv = lax.rsqrt(squares / (w1.shape[0] * w1.shape[2]) + norm_floor)
    proj[...] = (inv * part).astype(jnp.bfloat16)


def last_kernel(tp, mixed, outw, near, final, mg, we, xg, xo, send, recv, xsend, xrecv, osend, orecv):
    lanes = Lanes(tp)
    current = project_out(lanes, tp, 1, mixed, outw, near, mg, we, send, recv)
    mine, lane = current.shape[0], current.shape[1] // 2
    d, per = lanes.d, tp // 2
    for k in range(2):
        xg[k, lanes.t] = current[:, k * lane : (k + 1) * lane]

    def hand(half, block):
        place = lax.rem(block, per)
        return remote(xg.at[half, block], xo.at[half, place], osend.at[half, place], orecv.at[half, place], lanes.t, 1 - d)

    def arrived(half, block):
        @pl.when(block // per == 1 - d)
        def _():
            hand(half, block).start()

    arrived(0, lanes.t)
    arrived(1, lanes.t)
    gather(lanes, xg, xsend, xrecv, arrived=arrived)
    for j in range(per):
        for k in range(2):
            at = (2 * j + k) * lane
            final[pl.ds(pl.multiple_of(d * mine, mine), mine), at : at + lane] = xg[k, d * per + j]
    for j in range(per):
        for k in range(2):
            hand(k, (1 - d) * per + j).wait_recv()
    for j in range(per):
        for k in range(2):
            at = (2 * j + k) * lane
            final[pl.ds(pl.multiple_of((1 - d) * mine, mine), mine), at : at + lane] = xo[k, j]
    for j in range(per):
        for k in range(2):
            hand(k, (1 - d) * per + j).wait_send()


def fast(tp, tokens, norm_gain, projections, decay_base, group_gain, output_proj, state):
    rows, feats = tokens.shape
    mine, per = rows // 2, tp // 2
    cols = feats // per
    width = 6 * HEAD
    lines = HEAD * HEAD // (2 * HEAD)
    bf, f32 = jnp.bfloat16, jnp.float32
    shape = jax.ShapeDtypeStruct
    dma = pltpu.SemaphoreType.DMA
    vm, anywhere = pl.BlockSpec(memory_space=pltpu.VMEM), pl.BlockSpec(memory_space=pl.ANY)
    turned = [jnp.swapaxes(w, 1, 2) for w in projections]
    flat = state.reshape(LAYERS, mine * lines, 2 * HEAD)

    def params(number):
        return pltpu.CompilerParams(collective_id=number, has_side_effects=True, vmem_limit_bytes=VMEM_LIMIT)

    proj, near, w1, gain1, outw = pl.pallas_call(
        functools.partial(first_kernel, tp),
        out_shape=(
            shape((mine, width), bf), shape((mine, cols), bf), shape((2, width, feats), bf),
            shape((2, LAYERS, feats), f32), shape((tp, LAYERS, HEAD, cols), bf),
        ),
        in_specs=[anywhere, vm] + [anywhere] * 7,
        out_specs=(vm,) * 5,
        scratch_shapes=[
            pltpu.VMEM((rows, feats), bf), pltpu.VMEM((width, feats), bf), pltpu.VMEM((rows, width + 128), f32),
            pltpu.VMEM((mine, width + 128), f32), dma((13,)), dma((9,)), dma((9,)), dma((per,)), dma((tp,)),
            dma((tp,)), dma((tp,)),
        ],
        compiler_params=params(0),
        name="first",
    )(tokens, norm_gain, *turned, output_proj)

    seqs = min(mine, 32)

    def recur(layer, proj, filled):
        extra = [] if filled is None else [filled]
        return pl.pallas_call(
            state_kernel,
            grid=(mine // seqs,),
            out_shape=(shape(flat.shape, f32), shape((mine, HEAD), bf)),
            in_specs=[
                pl.BlockSpec((seqs, width), lambda i: (i, 0)),
                pl.BlockSpec((1, HEAD), lambda i: (0, 0)),
                pl.BlockSpec((1, HEAD), lambda i: (0, 0)),
                pl.BlockSpec((1, seqs * lines, 2 * HEAD), lambda i: (layer, i, 0)),
            ] + [anywhere] * len(extra),
            out_specs=(
                pl.BlockSpec((1, seqs * lines, 2 * HEAD), lambda i: (layer, i, 0)),
                pl.BlockSpec((seqs, HEAD), lambda i: (i, 0)),
            ),
            input_output_aliases={4: 0} if extra else {},
            compiler_params=pltpu.CompilerParams(vmem_limit_bytes=VMEM_LIMIT),
            name=f"state{layer}",
        )(proj, decay_base[layer : layer + 1], group_gain[layer : layer + 1], flat, *extra)

    filled, mixed = recur(0, proj, None)
    common = [pltpu.VMEM((2, tp, mine // 4, 2 * HEAD), bf), pltpu.VMEM((tp * 2 * HEAD, 2 * cols), bf),
              pltpu.VMEM((2, tp, mine, cols // 2), bf)]
    sems = [dma((2, tp)), dma((2, tp)), dma((2, tp)), dma((2, tp))]
    proj, near = pl.pallas_call(
        functools.partial(middle_kernel, tp),
        out_shape=(shape((mine, width), bf), shape((mine, cols), bf)),
        in_specs=[vm] * 3 + [anywhere, vm],
        out_specs=(vm,) * 2,
        scratch_shapes=common + sems + [pltpu.VMEM(w1.shape, bf), dma],
        compiler_params=params(1),
        name="middle",
    )(mixed, outw, near, w1, gain1)
    filled, mixed = recur(1, proj, filled)
    final = pl.pallas_call(
        functools.partial(last_kernel, tp),
        out_shape=shape((rows, feats), bf),
        in_specs=[vm] * 3,
        out_specs=vm,
        scratch_shapes=common + [pltpu.VMEM((2, per, mine, cols // 2), bf)] + sems + [dma((2, per)), dma((2, per))],
        compiler_params=params(2),
        name="last",
    )(mixed, outw, near)
    return (final, filled.reshape(state.shape))


def step(tp, dp, tokens, norm_gain, *rest):
    projections, (decay_base, group_gain, output_proj, state) = rest[:6], rest[6:]
    rows, feats = tokens.shape
    fits = dp == 2 and tp % 8 == 0 and state.shape[2] == 1 and state.shape[1] % 64 == 0 and (feats * dp // tp) % 256 == 0
    if fits:
        return fast(tp, tokens, norm_gain, projections, decay_base, group_gain, output_proj, state)
    return shards(tokens, norm_gain, *rest)


def solution(mesh):
    return jax.shard_map(
        functools.partial(step, mesh.shape["tp"], mesh.shape["dp"]),
        mesh=mesh,
        in_specs=(
            P(None, "dp"),
            P(None, "dp"),
            P(None, "dp", "tp"),
            P(None, "dp", "tp"),
            P(None, "dp", "tp"),
            P(None, "dp", "tp"),
            P(None, "dp", "tp"),
            P(None, "dp", "tp"),
            P(None, "tp"),
            P(None, "tp"),
            P(None, "tp", "dp"),
            P(None, "dp", "tp", None),
        ),
        out_specs=(P(None, "dp"), P(None, "dp", "tp", None)),
        check_vma=False,
    )
```
